32 devices in a mesh: grp: 2 (over y), fs: 4 (over z), tp: 4 (over x, core).
Axes of the slice: x: 2, y: 2, z: 4, core: 2. Of those that a mesh axis runs over, the one named last changes fastest.
Arguments:
- tokens: bfloat16 [2048, 4096], P(('grp', 'tp')), parts along dimension 0, may hold values from -6 to 6
- routes: int32 [2048, 2], P(('grp', 'tp')), parts along dimension 0, may hold values from 0 to 7, all different within a row; in each aligned block of 256 rows (0 to 255, 256 to 511, ...) at most 128 rows name the same one
- route_weight: float32 [2048, 2], P(('grp', 'tp')), parts along dimension 0, may hold values from 0.2 to 1
- norm_gain: float32 [4096], P('fs'), may hold values from 0.1 to 1.9
- gate_train: float32 [8, 4096, 2048], P(None, 'fs', 'tp'), may hold values from -0.09375 to 0.09375
- up_train: float32 [8, 4096, 2048], P(None, 'fs', 'tp'), may hold values from -0.09375 to 0.09375
- down_train: float32 [8, 2048, 4096], P(None, 'fs', 'tp'), may hold values from -0.125 to 0.125
Outputs:
- gate_serve: bfloat16 [16, 4096, 2048], P(('grp', 'tp'), None, 'fs'), parts along dimension 0
- up_serve: bfloat16 [16, 4096, 2048], P(('grp', 'tp'), None, 'fs'), parts along dimension 0
- down_serve: bfloat16 [16, 2048, 4096], P(('grp', 'tp'), 'fs'), parts along dimension 0
- moe_out: bfloat16 [2048, 4096], P(('grp', 'tp'), 'fs'), parts along dimension 0
The draws below stay inside these ranges and needn't reach their ends.
There are 2 independent parts, one for each index of `grp`. The reference program is written for one: setup_inputs(seed, part) draws one part's arguments, and reference() takes and returns one part's arrays. A program takes and returns all parts, laid end to end along the dimension named above; an argument that names none is the same for every part. Nothing has to cross between parts.
Inputs may be any that keep to these rules, and one draw needn't show every extreme that they name: `routes`: within the 256 rows of each device (aligned blocks), no expert is named by more than 128 rows, a bound that some block reaches; the two experts of a row differ; every expert is named somewhere.
All inputs are finite; a program needn't handle non-finite values.
Results may differ from the reference program's by a relative error of at most 0.0076.
Values may be sent and summed in bfloat16 or wider, within the bound.
A program may use at most 192 MiB of HBM per device.

```python
import math
import jax
import jax.numpy as jnp
import numpy as np
from jax import lax

D = 4096
FF = 2048
EXPERTS = 8
TOK_DEV = 256
CAP = 128
TOKENS = 1024


def block_scale(stream_key, shape, pieces, low, high):
    def one(axis_at, shards_of):
        steps = jax.random.uniform(jax.random.fold_in(jax.random.fold_in(stream_key, 6), axis_at), (shards_of,), jnp.float32, low / len(pieces), high / len(pieces))
        return jnp.repeat(jnp.exp(steps), shape[axis_at] // shards_of).reshape((-1,) + (1,) * (len(shape) - axis_at - 1))

    level = one(*pieces[0])
    for cut in pieces[1:]:
        level = level * one(*cut)
    return level


def routed_block(own_key, own, number, rows, number_of, top, reach, skew):
    order = jax.random.permutation(own_key, number_of)
    crowded, common = shares(number_of, rows * top, reach, skew, True), shares(number_of, rows * top, reach, skew, False)
    places = jnp.arange(number_of)

    def named(sizes, offset_by):
        used = int((sizes > 0).sum())
        fixed = max(1, used // 4)
        passed = fixed + (places - fixed + offset_by * (used - fixed)) % max(1, number_of - fixed)
        return jnp.zeros((number_of,), jnp.int32).at[order[jnp.where(places < fixed, places, passed)]].set(jnp.asarray(sizes, jnp.int32))

    sizes = jnp.where(number % 4 == 0, named(crowded, number // 4), named(common, number - number // 4 - 1))
    mixed = jax.random.permutation(jax.random.fold_in(own, 3), number_of)
    giver, taker = mixed[0:number_of // 2 * 2:2], mixed[1:number_of // 2 * 2:2]
    margin = jnp.minimum(sizes[giver] - 1, reach - sizes[taker]) // 2
    margin = jnp.where((giver == order[0]) | (taker == order[0]) | (sizes[taker] == 0), 0, jnp.maximum(margin, 0))
    passed = jax.random.randint(jax.random.fold_in(own, 4), (number_of // 2,), 0, 1 << 20) % (margin + 1)
    sizes = sizes.at[giver].add(-passed).at[taker].add(passed)
    items = jnp.searchsorted(jnp.cumsum(sizes), jnp.arange(rows * top), side="right").astype(jnp.int32)
    grid = items.reshape(top, rows).T
    grid = grid[jax.random.permutation(jax.random.fold_in(own, 1), rows)]
    offset_by = jax.random.randint(jax.random.fold_in(own, 2), (rows, 1), 0, top)
    return jnp.take_along_axis(grid, (jnp.arange(top)[None, :] + offset_by) % top, axis=1)


def shares(amount, total, reach, skew, full):
    weights = [(1 << 20) // math.isqrt(standing ** skew) + 1 for standing in range(1, amount + 1)]
    largest = reach if full else min(reach, max(-(-total // amount), total * weights[0] // sum(weights)))
    least = 1 if total - largest >= amount - 1 else 0
    counts, rest = [largest] + [least] * (amount - 1), total - largest - least * (amount - 1)
    while rest > 0:
        free = [i for i in range(1, amount) if counts[i] < largest] or [i for i in range(1, amount) if counts[i] < reach]
        mass, remaining = sum([weights[i] for i in free]), rest
        for i in free:
            addition = min(reach - counts[i], max(1, remaining * weights[i] // mass), rest)
            counts[i] = counts[i] + addition
            rest = rest - addition
    return np.array(counts)


def centred(rng, extent, scale, bound, split=(), kind=jnp.bfloat16):
    values = scale * jax.random.normal(rng, extent, jnp.float32)
    if split:
        values = values * block_scale(rng, extent, split, -0.22, 0.18)
    return jnp.clip(values, -bound, bound).astype(kind)


def setup_inputs(seed: int = 0, part: int = 0) -> dict:
    key_list = jax.random.split(jax.random.key(seed), 8)
    part_splits = jax.random.split(jax.random.fold_in(key_list[7], part), 8)
    tokens = centred(part_splits[0], (TOKENS, D), 1.0, 6.0, ((0, 4),))
    routes_keys = jax.random.split(jax.random.fold_in(part_splits[1], 1), TOKENS // TOK_DEV)
    routes_turns = jax.random.permutation(jax.random.fold_in(part_splits[1], 3), TOKENS // TOK_DEV)
    routes = jax.vmap(lambda own, number: routed_block(jax.random.fold_in(part_splits[1], 2), own, number, TOK_DEV, EXPERTS, 2, CAP, 1))(routes_keys, routes_turns).reshape((TOKENS, 2))
    route_weight = jnp.clip(0.2 + 0.8 * jax.random.uniform(part_splits[2], (TOKENS, 2), jnp.float32) ** block_scale(part_splits[2], (TOKENS, 2), ((0, 4),), -0.2, 0.2), 0.2, 1.0)
    norm_gain = jnp.clip(1.0 + 0.18 * jax.random.normal(key_list[3], (D,), jnp.float32), 0.1, 1.9)
    gate_train = centred(key_list[4], (EXPERTS, D, FF), D ** -0.5, 0.09375, ((1, 4), (2, 4)), jnp.float32)
    up_train = centred(key_list[5], (EXPERTS, D, FF), D ** -0.5, 0.09375, ((1, 4), (2, 4)), jnp.float32)
    down_train = centred(key_list[6], (EXPERTS, FF, D), FF ** -0.5, 0.125, ((1, 4), (2, 4)), jnp.float32)
    return {"tokens": tokens, "routes": routes, "route_weight": route_weight, "norm_gain": norm_gain, "gate_train": gate_train, "up_train": up_train, "down_train": down_train}


def reference(tokens, routes, route_weight, norm_gain, gate_train, up_train, down_train):
    gate_serve = (norm_gain[None, :, None] * gate_train).astype(jnp.bfloat16)
    up_serve = (norm_gain[None, :, None] * up_train).astype(jnp.bfloat16)
    down_serve = down_train.astype(jnp.bfloat16)

    def expert_step(total, inputs):
        index, gate_one, up_one, down_one = inputs
        gate_h = jnp.dot(tokens, gate_one, preferred_element_type=jnp.float32)
        up_h = jnp.dot(tokens, up_one, preferred_element_type=jnp.float32)
        hidden = (jax.nn.silu(gate_h) * up_h).astype(jnp.bfloat16)
        result = jnp.dot(hidden, down_one, preferred_element_type=jnp.float32).astype(jnp.bfloat16)
        result = lax.optimization_barrier(result)
        weight = jnp.sum(jnp.where(routes == index, route_weight, jnp.zeros_like(route_weight)), axis=1)
        return total + weight[:, None] * result.astype(jnp.float32), None

    start = jnp.zeros((tokens.shape[0], tokens.shape[1]), jnp.float32)
    total, _ = lax.scan(expert_step, start,
                        (jnp.arange(EXPERTS, dtype=jnp.int32), gate_serve, up_serve, down_serve))
    return gate_serve, up_serve, down_serve, total.astype(jnp.bfloat16)
```

```python
import functools

import jax
import jax.numpy as jnp
from jax import lax
from jax.experimental import pallas as pl
from jax.experimental.pallas import tpu as pltpu
from jax.sharding import PartitionSpec as P

EXPERTS = 8
CAP = 128
MESH = pl.DeviceIdType.MESH


def interleaved(n):
    half = n // 2
    return [k // 2 + (k % 2) * half for k in range(n)]


def handoff(ngrp, nfs, ntp, gate, up, down, tok, gate_out, up_out, down_out, tok_out,
            stage, stage_sem, send_sem, recv_sem, dsend, drecv, tsend, trecv):
    g, f, t = lax.axis_index("grp"), lax.axis_index("fs"), lax.axis_index("tp")
    ratio = nfs // ntp
    local = gate_out.shape[0]
    rows = gate.shape[1]
    half = rows // 2
    width = gate_out.shape[2]
    other = 1 - g
    owner = f // ratio
    order = interleaved(ntp)

    barrier = pltpu.get_barrier_semaphore()

    def greet(dev, skip):
        @pl.when(jnp.logical_not(skip))
        def _():
            pl.semaphore_signal(barrier, inc=1, device_id=dev, device_id_type=MESH)

    for q in range(ratio):
        for k in range(ntp):
            greet((g, t * ratio + q, k), (f == t * ratio + q) & (t == k))
    for k in range(nfs):
        greet((g, k, owner), (f == k) & (t == owner))
    for k in range(1, ntp):
        greet((g, f, (t + k) % ntp), False)
    greet((other, f, t), False)
    total = ratio * ntp + nfs + ntp - 1 + 1
    me = (t == owner).astype(jnp.int32)
    pl.semaphore_wait(barrier, total - 2 * me)

    def chunk(src, out, dev_f, dev_t, q, l, h, m):
        e = dev_t * local + l
        return pltpu.make_async_remote_copy(
            src_ref=src.at[e, pl.ds(h * half, half), pl.ds(q * width, width)],
            dst_ref=out.at[l, pl.ds(f * rows + h * half, half), :],
            send_sem=send_sem.at[m, q, dev_t, l, h],
            recv_sem=recv_sem.at[m, l, f, h],
            device_id=(g, dev_f, dev_t), device_id_type=MESH)

    mats = ((gate, gate_out), (up, up_out))
    for m, (src, out) in enumerate(mats):
        for k in order:
            for l in range(local):
                for q in range(ratio):
                    dev_f, dev_t = t * ratio + q, (t + k) % ntp
                    for h in range(2):
                        send = (dev_f == f) | (g == h)
                        mine = (dev_f == f) & (dev_t == t)

                        @pl.when(send & jnp.logical_not(mine))
                        def _(src=src, out=out, q=q, l=l, h=h, m=m, dev_f=dev_f, dev_t=dev_t):
                            chunk(src, out, dev_f, dev_t, q, l, h, m).start()

    def tok_copy(k):
        n_tok = tok.shape[0]
        return pltpu.make_async_remote_copy(
            src_ref=tok, dst_ref=tok_out.at[pl.ds(t * n_tok, n_tok), :],
            send_sem=tsend.at[k - 1], recv_sem=trecv.at[k - 1],
            device_id=(g, f, (t + k) % ntp), device_id_type=MESH)

    for k in range(1, ntp):
        tok_copy(k).start()

    dcols = down.shape[2]

    def down_copy(k, l):
        return pltpu.make_async_remote_copy(
            src_ref=down.at[((t + k) % ntp) * local + l],
            dst_ref=down_out.at[l, :, pl.ds(t * dcols, dcols)],
            send_sem=dsend.at[k - 1, l], recv_sem=drecv.at[k - 1, l],
            device_id=(g, f, (t + k) % ntp), device_id_type=MESH)

    for k in range(1, ntp):
        for l in range(local):
            down_copy(k, l).start()

    def through(src, dst, buf, sem):
        load = pltpu.make_async_copy(src, buf, sem)
        load.start()
        load.wait()
        store = pltpu.make_async_copy(buf, dst, sem)
        store.start()
        store.wait()

    n_tok = tok.shape[0]
    through(tok, tok_out.at[pl.ds(t * n_tok, n_tok), :], stage[0], stage_sem)
    for l in range(local):
        through(down.at[t * local + l], down_out.at[l, :, pl.ds(t * dcols, dcols)],
                stage[1], stage_sem)

    @pl.when(t == owner)
    def _():
        q = f - t * ratio
        for m, (src, out) in enumerate(mats):
            for l in range(local):
                for qq in range(ratio):
                    @pl.when(q == qq)
                    def _(src=src, out=out, l=l, qq=qq):
                        through(src.at[t * local + l, :, pl.ds(qq * width, width)],
                                out.at[l, pl.ds(f * rows, rows), :], stage[2], stage_sem)

    def forward(m, out, l, fs_src):
        view = out.at[l, pl.ds(fs_src * rows + g * half, half), :]
        return pltpu.make_async_remote_copy(
            src_ref=view, dst_ref=view,
            send_sem=send_sem.at[m, ratio, fs_src % ntp, l, fs_src // ntp],
            recv_sem=recv_sem.at[m, l, fs_src, g],
            device_id=(other, f, t), device_id_type=MESH)

    def arrived(m, out, l, fs_src, h):
        view = out.at[l, pl.ds(fs_src * rows + h * half, half), :]
        pltpu.make_async_copy(view, view, recv_sem.at[m, l, fs_src, h]).wait()

    for m, (src, out) in enumerate(mats):
        for l in range(local):
            for d in range(1, nfs):
                fs_src = (f + d) % nfs
                arrived(m, out, l, fs_src, g)
                forward(m, out, l, fs_src).start()
    for m, (src, out) in enumerate(mats):
        for l in range(local):
            for d in range(1, nfs):
                arrived(m, out, l, (f + d) % nfs, other)

            @pl.when(t != owner)
            def _(m=m, out=out, l=l):
                for h in range(2):
                    arrived(m, out, l, f, h)
    for k in range(1, ntp):
        tok_copy(k).wait()
        for l in range(local):
            down_copy(k, l).wait()
    for m, (src, out) in enumerate(mats):
        for l in range(local):
            for d in range(1, nfs):
                forward(m, out, l, (f + d) % nfs).wait_send()
            for k in range(ntp):
                for q in range(ratio):
                    dev_f, dev_t = t * ratio + q, (t + k) % ntp
                    for h in range(2):
                        @pl.when(((dev_f == f) | (g == h)) & ((dev_f != f) | (dev_t != t)))
                        def _(src=src, out=out, q=q, l=l, h=h, m=m, dev_f=dev_f, dev_t=dev_t):
                            chunk(src, out, dev_f, dev_t, q, l, h, m).wait_send()


def move_weights(gate, up, down, tokens, nfs, ntp):
    local = EXPERTS // ntp
    width = gate.shape[2] * ntp // nfs
    rows, dcols = gate.shape[1], down.shape[2]
    dma = pltpu.SemaphoreType.DMA
    any_spec = pl.BlockSpec(memory_space=pl.ANY)
    bf = jnp.bfloat16
    ratio = nfs // ntp
    return pl.pallas_call(
        functools.partial(handoff, 2, nfs, ntp),
        out_shape=(
            jax.ShapeDtypeStruct((local, rows * nfs, width), bf),
            jax.ShapeDtypeStruct((local, rows * nfs, width), bf),
            jax.ShapeDtypeStruct((local, down.shape[1], dcols * ntp), bf),
            jax.ShapeDtypeStruct((tokens.shape[0] * ntp, tokens.shape[1]), bf),
        ),
        in_specs=[any_spec] * 4,
        out_specs=(any_spec,) * 4,
        scratch_shapes=[
            [pltpu.VMEM(tokens.shape, bf), pltpu.VMEM(down.shape[1:], bf),
             pltpu.VMEM((rows, width), bf)],
            dma,
            dma((2, ratio + 1, ntp, local, max(2, ratio))),
            dma((2, local, nfs, 2)),
            dma((ntp - 1, local)), dma((ntp - 1, local)),
            dma((ntp - 1,)), dma((ntp - 1,)),
        ],
        compiler_params=pltpu.CompilerParams(collective_id=0, has_side_effects=True),
    )(gate, up, down, tokens)


def per_device(tokens, routes, route_weight, norm_gain, gate_train, up_train, down_train):
    nfs, ntp = lax.axis_size("fs"), lax.axis_size("tp")
    t = lax.axis_index("tp")
    bf = jnp.bfloat16
    gate_cast = (norm_gain[None, :, None] * gate_train).astype(bf)
    up_cast = (norm_gain[None, :, None] * up_train).astype(bf)
    down_cast = down_train.astype(bf)
    gate_serve, up_serve, down_serve, tok_all = move_weights(
        gate_cast, up_cast, down_cast, tokens, nfs, ntp)
    local = EXPERTS // ntp
    n_tok = tokens.shape[0]
    routes_all = lax.all_gather(routes, "tp", axis=0)
    weight_all = lax.all_gather(route_weight, "tp", axis=0)
    expert_ids = jnp.arange(EXPERTS, dtype=jnp.int32)
    named = routes_all[None] == expert_ids[:, None, None, None]
    chosen = jnp.any(named, axis=3)
    weight_e = jnp.sum(jnp.where(named, weight_all[None], 0.0), axis=3)
    count = chosen.astype(jnp.int32)
    slot = jnp.cumsum(count, axis=2) - count
    slot_ids = jnp.arange(CAP, dtype=jnp.int32)
    select = (chosen[:, :, None, :] & (slot[:, :, None, :] == slot_ids[None, None, :, None])).astype(bf)
    mine = lax.dynamic_slice_in_dim(select, t * local, local, axis=0)
    weight_mine = lax.dynamic_slice_in_dim(weight_e, t * local, local, axis=0)
    gate_h = jnp.einsum("td,ldf->ltf", tok_all, gate_serve, preferred_element_type=jnp.float32)
    up_h = jnp.einsum("td,ldf->ltf", tok_all, up_serve, preferred_element_type=jnp.float32)
    hidden = jax.nn.silu(gate_h) * up_h * weight_mine.reshape(local, -1)[:, :, None]
    hidden = hidden.astype(bf).reshape(local, ntp, n_tok, -1)
    packed = jnp.einsum("lbst,lbtf->lbsf", mine, hidden, preferred_element_type=jnp.float32).astype(bf)
    packed = lax.all_gather(packed, "tp", axis=0, tiled=True)
    dense = jnp.einsum("ebst,ebsf->btef", select, packed, preferred_element_type=jnp.float32).astype(bf)
    partial = jnp.dot(
        dense.reshape(ntp * n_tok, -1), down_cast.reshape(-1, down_cast.shape[2]),
        preferred_element_type=jnp.float32).astype(bf)
    ratio = nfs // ntp
    partial = partial.reshape(ntp, n_tok, ratio, -1)
    partial = lax.all_to_all(partial, "tp", split_axis=0, concat_axis=0, tiled=True)
    partial = partial.transpose(0, 2, 1, 3).reshape(nfs, n_tok, -1)
    partial = lax.all_to_all(partial, "fs", split_axis=0, concat_axis=0, tiled=True)
    moe_out = jnp.sum(partial.astype(jnp.float32), axis=0).astype(bf)
    return (gate_serve, up_serve, down_serve, moe_out)


def solution(mesh):
    return jax.shard_map(
        per_device,
        mesh=mesh,
        in_specs=(
            P(("grp", "tp"), None),
            P(("grp", "tp"), None),
            P(("grp", "tp"), None),
            P("fs"),
            P(None, "fs", "tp"),
            P(None, "fs", "tp"),
            P(None, "fs", "tp"),
        ),
        out_specs=(
            P(("grp", "tp"), None, "fs"),
            P(("grp", "tp"), None, "fs"),
            P(("grp", "tp"), "fs", None),
            P(("grp", "tp"), "fs"),
        ),
        check_vma=False,
    )
```

```python
import functools

import jax
import jax.numpy as jnp
from jax import lax
from jax.experimental import pallas as pl
from jax.experimental.pallas import tpu as pltpu
from jax.sharding import PartitionSpec as P

EXPERTS = 8
CAP = 128
MESH = pl.DeviceIdType.MESH


def handoff(nfs, ntp, gate, up, down, tok, gate_out, up_out, down_out, tok_out, relay,
            stage, stage_sem, send_sem, recv_sem, hand_sem, pass_send, pass_recv,
            dsend, drecv, tsend, trecv):
    g, f, t = lax.axis_index("grp"), lax.axis_index("fs"), lax.axis_index("tp")
    ratio = nfs // ntp
    chips = ntp // 2
    local = gate_out.shape[0]
    rows = gate.shape[1]
    half = rows // 2
    width = gate_out.shape[2]
    other = 1 - g
    owner = f // ratio
    base = (t // 2) * 2
    mate = base + 1 - t % 2

    barrier = pltpu.get_barrier_semaphore()

    def greet(dev, skip):
        @pl.when(jnp.logical_not(skip))
        def _():
            pl.semaphore_signal(barrier, inc=1, device_id=dev, device_id_type=MESH)

    for j in range(chips):
        for q in range(ratio):
            for tc in range(2):
                dev_f = ((t + ntp - 2 * j) % ntp) * ratio + q
                greet((g, dev_f, base + tc), (f == dev_f) & (t == base + tc))
    for k in range(nfs):
        greet((g, k, base + owner % 2), (f == k) & (t % 2 == owner % 2))
    for k in range(1, ntp):
        greet((g, f, (t + k) % ntp), False)
    greet((other, f, t), False)
    me = (t % 2 == owner % 2).astype(jnp.int32)
    pl.semaphore_wait(barrier, 2 * nfs - 2 * me + ntp)

    mats = ((gate, gate_out), (up, up_out))
    steps = [(m, l) for m in range(2) for l in range(local)]

    def chunk(m, l, j, tc, q, h):
        src, out = mats[m]
        dev_t = ((t + 2 * j) % ntp) // 2 * 2 + tc
        return pltpu.make_async_remote_copy(
            src_ref=src.at[dev_t * local + l, pl.ds(h * half, half), pl.ds(q * width, width)],
            dst_ref=out.at[l, pl.ds(f * rows + h * half, half), :],
            send_sem=send_sem.at[m, l, j, tc, q, h],
            recv_sem=recv_sem.at[m, l, f, h],
            device_id=(g, t * ratio + q, dev_t), device_id_type=MESH)

    def hop(m, l, j, tc, q):
        src, _ = mats[m]
        near = (t + 2 * j) % ntp
        return pltpu.make_async_remote_copy(
            src_ref=src.at[(near // 2 * 2 + tc) * local + l, pl.ds(g * half, half),
                           pl.ds(q * width, width)],
            dst_ref=relay.at[m, l, j - 1, tc, q],
            send_sem=send_sem.at[m, l, j, tc, q, 0],
            recv_sem=pass_recv.at[m, l, j - 1, tc, q],
            device_id=(g, f, near), device_id_type=MESH)

    def onward(m, l, j, tc, q):
        _, out = mats[m]
        came = (t + ntp - 2 * j) % ntp
        return pltpu.make_async_remote_copy(
            src_ref=relay.at[m, l, j - 1, tc, q],
            dst_ref=out.at[l, pl.ds(f * rows + g * half, half), :],
            send_sem=pass_send.at[m, l, j - 1, tc, q],
            recv_sem=recv_sem.at[m, l, f, g],
            device_id=(g, came * ratio + q, base + tc), device_id_type=MESH)

    def each_send(act):
        for m, l in steps:
            for tc in range(2):
                for j in range(chips):
                    for q in range(ratio):
                        far = t * ratio + q != f
                        if j == 0:
                            for h in range(2):
                                @pl.when((far & (g == h)) | (jnp.logical_not(far) & (base + tc != t)))
                                def _(h=h):
                                    act(chunk(m, l, j, tc, q, h))
                        else:
                            @pl.when(far)
                            def _():
                                act(hop(m, l, j, tc, q))

                            @pl.when(jnp.logical_not(far))
                            def _():
                                for h in range(2):
                                    act(chunk(m, l, j, tc, q, h))

    each_send(lambda copy: copy.start())

    n_tok = tok.shape[0]

    def tok_copy(j):
        return pltpu.make_async_remote_copy(
            src_ref=tok, dst_ref=tok_out.at[pl.ds(t * n_tok, n_tok), :],
            send_sem=tsend.at[0, j], recv_sem=trecv.at[t],
            device_id=(g, f, (t + 2 * j) % ntp if j else mate), device_id_type=MESH)

    def tok_view(who):
        return tok_out.at[pl.ds(who * n_tok, n_tok), :]

    def tok_share(j):
        came = (t + ntp - 2 * j) % ntp
        return pltpu.make_async_remote_copy(
            src_ref=tok_view(came), dst_ref=tok_view(came),
            send_sem=tsend.at[1, j], recv_sem=trecv.at[came],
            device_id=(g, f, mate), device_id_type=MESH)

    def tok_arrived(who):
        pltpu.make_async_copy(tok_view(who), tok_view(who), trecv.at[who]).wait()

    for j in range(chips):
        tok_copy(j).start()

    dcols = down.shape[2]

    def down_copy(k, l):
        return pltpu.make_async_remote_copy(
            src_ref=down.at[((t + k) % ntp) * local + l],
            dst_ref=down_out.at[l, :, pl.ds(t * dcols, dcols)],
            send_sem=dsend.at[k - 1, l], recv_sem=drecv.at[k - 1, l],
            device_id=(g, f, (t + k) % ntp), device_id_type=MESH)

    for k in range(1, ntp):
        for l in range(local):
            down_copy(k, l).start()

    def through(src, dst, buf, sem):
        load = pltpu.make_async_copy(src, buf, sem)
        load.start()
        load.wait()
        store = pltpu.make_async_copy(buf, dst, sem)
        store.start()
        store.wait()

    through(tok, tok_view(t), stage[0], stage_sem)
    for l in range(local):
        through(down.at[t * local + l], down_out.at[l, :, pl.ds(t * dcols, dcols)],
                stage[1], stage_sem)

    @pl.when(t == owner)
    def _():
        for m, (src, out) in enumerate(mats):
            for l in range(local):
                for q in range(ratio):
                    @pl.when(f - t * ratio == q)
                    def _():
                        through(src.at[t * local + l, :, pl.ds(q * width, width)],
                                out.at[l, pl.ds(f * rows, rows), :], stage[2], stage_sem)

    def relayed(act):
        def step(m, l):
            for tc in range(2):
                for j in range(1, chips):
                    for q in range(ratio):
                        came = (t + ntp - 2 * j) % ntp

                        @pl.when(came * ratio + q != f)
                        def _():
                            act(m, l, j, tc, q)
        return step

    def pass_on(m, l, j, tc, q):
        view = relay.at[m, l, j - 1, tc, q]
        pltpu.make_async_copy(view, view, pass_recv.at[m, l, j - 1, tc, q]).wait()
        onward(m, l, j, tc, q).start()

    def forward(m, l, fs_src):
        view = mats[m][1].at[l, pl.ds(fs_src * rows + g * half, half), :]
        return pltpu.make_async_remote_copy(
            src_ref=view, dst_ref=view,
            send_sem=hand_sem.at[m, l, fs_src],
            recv_sem=recv_sem.at[m, l, fs_src, g],
            device_id=(other, f, t), device_id_type=MESH)

    def arrived(m, l, fs_src, h):
        view = mats[m][1].at[l, pl.ds(fs_src * rows + h * half, half), :]
        pltpu.make_async_copy(view, view, recv_sem.at[m, l, fs_src, h]).wait()

    def hand_on(m, l):
        for d in range(1, nfs):
            fs_src = (f + d) % nfs
            arrived(m, l, fs_src, g)
            forward(m, l, fs_src).start()

    ahead = relayed(pass_on)
    ahead(*steps[0])
    for i, step in enumerate(steps):
        if i + 1 < len(steps):
            ahead(*steps[i + 1])
        if i + 1 == len(steps):
            for j in range(1, chips):
                tok_arrived((t + ntp - 2 * j) % ntp)
                tok_share(j).start()
        hand_on(*step)

    for m, l in steps:
        for d in range(1, nfs):
            arrived(m, l, (f + d) % nfs, other)

        @pl.when(t != owner)
        def _():
            for h in range(2):
                arrived(m, l, f, h)
    tok_arrived(mate)
    for j in range(1, chips):
        tok_arrived((mate + ntp - 2 * j) % ntp)
        tok_share(j).wait_send()
    for j in range(chips):
        tok_copy(j).wait_send()
    for k in range(1, ntp):
        for l in range(local):
            down_copy(k, l).wait()
    each_send(lambda copy: copy.wait_send())
    passed = relayed(lambda *which: onward(*which).wait_send())
    for m, l in steps:
        passed(m, l)
        for d in range(1, nfs):
            forward(m, l, (f + d) % nfs).wait_send()


def move_weights(gate, up, down, tokens, nfs, ntp):
    local = EXPERTS // ntp
    width = gate.shape[2] * ntp // nfs
    rows, dcols = gate.shape[1], down.shape[2]
    dma = pltpu.SemaphoreType.DMA
    any_spec = pl.BlockSpec(memory_space=pl.ANY)
    bf = jnp.bfloat16
    ratio = nfs // ntp
    chips = ntp // 2
    passes = (2, local, chips - 1, 2, ratio)
    return pl.pallas_call(
        functools.partial(handoff, nfs, ntp),
        out_shape=(
            jax.ShapeDtypeStruct((local, rows * nfs, width), bf),
            jax.ShapeDtypeStruct((local, rows * nfs, width), bf),
            jax.ShapeDtypeStruct((local, down.shape[1], dcols * ntp), bf),
            jax.ShapeDtypeStruct((tokens.shape[0] * ntp, tokens.shape[1]), bf),
            jax.ShapeDtypeStruct((*passes, rows // 2, width), bf),
        ),
        in_specs=[any_spec] * 4,
        out_specs=(any_spec,) * 5,
        scratch_shapes=[
            [pltpu.VMEM(tokens.shape, bf), pltpu.VMEM(down.shape[1:], bf),
             pltpu.VMEM((rows, width), bf)],
            dma,
            dma((2, local, chips, 2, ratio, 2)),
            dma((2, local, nfs, 2)),
            dma((2, local, nfs)),
            dma(passes), dma(passes),
            dma((ntp - 1, local)), dma((ntp - 1, local)),
            dma((2, chips)), dma((ntp,)),
        ],
        compiler_params=pltpu.CompilerParams(collective_id=0, has_side_effects=True),
    )(gate, up, down, tokens)


def per_device(tokens, routes, route_weight, norm_gain, gate_train, up_train, down_train):
    nfs, ntp = lax.axis_size("fs"), lax.axis_size("tp")
    t = lax.axis_index("tp")
    bf = jnp.bfloat16
    gate_cast = (norm_gain[None, :, None] * gate_train).astype(bf)
    up_cast = (norm_gain[None, :, None] * up_train).astype(bf)
    down_cast = down_train.astype(bf)
    gate_serve, up_serve, down_serve, tok_all, _ = move_weights(
        gate_cast, up_cast, down_cast, tokens, nfs, ntp)
    local = EXPERTS // ntp
    n_tok = tokens.shape[0]
    routing = jnp.concatenate([routes.astype(jnp.float32), route_weight], axis=1)
    routing = lax.all_gather(routing, "tp", axis=0)
    routes_all = routing[:, :, :2].astype(jnp.int32)
    weight_all = routing[:, :, 2:]
    expert_ids = jnp.arange(EXPERTS, dtype=jnp.int32)
    named = routes_all[None] == expert_ids[:, None, None, None]
    chosen = jnp.any(named, axis=3)
    weight_e = jnp.sum(jnp.where(named, weight_all[None], 0.0), axis=3)
    count = chosen.astype(jnp.int32)
    slot = jnp.cumsum(count, axis=2) - count
    slot_ids = jnp.arange(CAP, dtype=jnp.int32)
    select = (chosen[:, :, None, :] & (slot[:, :, None, :] == slot_ids[None, None, :, None])).astype(bf)
    mine = lax.dynamic_slice_in_dim(select, t * local, local, axis=0)
    weight_mine = lax.dynamic_slice_in_dim(weight_e, t * local, local, axis=0)
    gate_h = jnp.einsum("td,ldf->ltf", tok_all, gate_serve, preferred_element_type=jnp.float32)
    up_h = jnp.einsum("td,ldf->ltf", tok_all, up_serve, preferred_element_type=jnp.float32)
    hidden = jax.nn.silu(gate_h) * up_h * weight_mine.reshape(local, -1)[:, :, None]
    hidden = hidden.astype(bf).reshape(local, ntp, n_tok, -1)
    packed = jnp.einsum("lbst,lbtf->lbsf", mine, hidden, preferred_element_type=jnp.float32).astype(bf)
    packed = lax.all_gather(packed, "tp", axis=0, tiled=True)
    dense = jnp.einsum("ebst,ebsf->btef", select, packed, preferred_element_type=jnp.float32).astype(bf)
    partial = jnp.dot(
        dense.reshape(ntp * n_tok, -1), down_cast.reshape(-1, down_cast.shape[2]),
        preferred_element_type=jnp.float32).astype(bf)
    ratio = nfs // ntp
    partial = partial.reshape(ntp, n_tok, ratio, -1)
    partial = lax.all_to_all(partial, "tp", split_axis=0, concat_axis=0, tiled=True)
    partial = partial.transpose(0, 2, 1, 3).reshape(nfs, n_tok, -1)
    partial = lax.all_to_all(partial, "fs", split_axis=0, concat_axis=0, tiled=True)
    moe_out = jnp.sum(partial.astype(jnp.float32), axis=0).astype(bf)
    return (gate_serve, up_serve, down_serve, moe_out)


def solution(mesh):
    return jax.shard_map(
        per_device,
        mesh=mesh,
        in_specs=(
            P(("grp", "tp"), None),
            P(("grp", "tp"), None),
            P(("grp", "tp"), None),
            P("fs"),
            P(None, "fs", "tp"),
            P(None, "fs", "tp"),
            P(None, "fs", "tp"),
        ),
        out_specs=(
            P(("grp", "tp"), None, "fs"),
            P(("grp", "tp"), None, "fs"),
            P(("grp", "tp"), "fs", None),
            P(("grp", "tp"), "fs"),
        ),
        check_vma=False,
    )
```
